256 devices in a mesh: grp: 2 (over y), fs: 16 (over z), tp: 8 (over x, core).
Axes of the slice: x: 4, y: 2, z: 16, core: 2. Of those that a mesh axis runs over, the one named last changes fastest.
The devices are a block of a 4x16x16 slice.
Arguments:
- tokens: bfloat16 [12288, 2048], P(('grp', 'fs'), 'tp'), parts along dimension 0, may hold values from -25 to 25
- gain_first: float32 [2048], replicated, may hold values from 0.1 to 1.9
- gate_first: bfloat16 [2048, 5120], P('fs', 'tp'), may hold values from -0.125 to 0.125
- up_first: bfloat16 [2048, 5120], P('fs', 'tp'), may hold values from -0.125 to 0.125
- down_first: bfloat16 [5120, 2048], P('tp', 'fs'), may hold values from -0.078125 to 0.078125
- gain_mixer: float32 [2048], replicated, may hold values from 0.1 to 1.9
- outer_gate: bfloat16 [2048, 1024], P('fs', 'tp'), may hold values from -0.125 to 0.125
- inner_gate: bfloat16 [2048, 1024], P('fs', 'tp'), may hold values from -0.125 to 0.125
- conv_input: bfloat16 [2048, 1024], P('fs', 'tp'), may hold values from -0.125 to 0.125
- conv_taps: float32 [3, 1024], P(None, 'tp'), may hold values from -3.5 to 3.5
- mixer_out: bfloat16 [1024, 2048], P('tp', 'fs'), may hold values from -0.1875 to 0.1875
- gain_last: float32 [2048], replicated, may hold values from 0.1 to 1.9
- gate_last: bfloat16 [2048, 5120], P('fs', 'tp'), may hold values from -0.125 to 0.125
- up_last: bfloat16 [2048, 5120], P('fs', 'tp'), may hold values from -0.125 to 0.125
- down_last: bfloat16 [5120, 2048], P('tp', 'fs'), may hold values from -0.078125 to 0.078125
Outputs:
- layer_out: bfloat16 [12288, 2048], P(('grp', 'fs'), 'tp'), parts along dimension 0
The draws below stay inside these ranges and needn't reach their ends.
There are 2 independent parts, one for each index of `grp`. The reference program is written for one: setup_inputs(seed, part) draws one part's arguments, and reference() takes and returns one part's arrays. A program takes and returns all parts, laid end to end along the dimension named above; an argument that names none is the same for every part. Nothing has to cross between parts.
All inputs are finite; a program needn't handle non-finite values.
Results may differ from the reference program's by a relative error of at most 0.015.
Values may be sent and summed in bfloat16 or wider, within the bound.
A program may use at most 64 MiB of HBM per device.

```python
import math
import jax
import jax.numpy as jnp
from jax import lax

D = 2048
FF = 5120
SC = 1024
KERNEL = 3
SEQ_LEN = 64
TOKENS = 6144
N_TP = 8


def draw_tokens(key, part):
    row_count = TOKENS
    col_count = D
    key_base, key_row, key_col = jax.random.split(jax.random.fold_in(key, 11), 3)
    values_raw = jnp.clip(jax.random.normal(key_base, (row_count, col_count), jnp.float32), -4.0, 4.0)
    row_scale = jnp.exp(jax.random.uniform(key_row, (row_count, 1), jnp.float32, math.log(0.5), math.log(2.0)))
    rising = 0.5 * jnp.power(4.0, jnp.arange(col_count, dtype=jnp.float32) / col_count)
    jitter = jnp.exp(jax.random.uniform(key_col, (col_count,), jnp.float32, -0.4, 0.4))
    return (values_raw * row_scale * (rising * jitter)[None, :]).astype(jnp.bfloat16)


def block_levels(key, shape, cuts, smallest, top_value):
    loudness = 1.0
    for position, shards_of in cuts:
        draws = jax.random.uniform(jax.random.fold_in(jax.random.fold_in(key, 6), position), (shards_of,), jnp.float32, smallest / len(cuts), top_value / len(cuts))
        loudness = loudness * jnp.repeat(jnp.exp(draws), shape[position] // shards_of).reshape((-1,) + (1,) * (len(shape) - 1 - position))
    return loudness


def scatter_about(key, shape, spread, limit, pieces=(), kind=jnp.bfloat16):
    drawn = spread * jax.random.normal(key, shape, jnp.float32)
    if pieces:
        drawn = drawn * block_levels(key, shape, pieces, -0.22, 0.18)
    return jnp.clip(drawn, -limit, limit).astype(kind)


def setup_inputs(seed: int = 0, part: int = 0) -> dict:
    key_of = jax.random.split(jax.random.key(seed), 16)
    part_keys = jax.random.split(jax.random.fold_in(key_of[15], part), 16)
    tokens = draw_tokens(jax.random.fold_in(jax.random.fold_in(key_of[15], part), 71), part)
    gain_first = jnp.clip(1.0 + 0.18 * jax.random.normal(key_of[1], (D,), jnp.float32), 0.1, 1.9)
    gate_first = scatter_about(key_of[2], (D, FF), D ** -0.5, 0.125, ((0, 16), (1, 8)))
    up_first = scatter_about(key_of[3], (D, FF), D ** -0.5, 0.125, ((0, 16), (1, 8)))
    down_first = scatter_about(key_of[4], (FF, D), FF ** -0.5, 0.078125, ((0, 8), (1, 16)))
    gain_mixer = jnp.clip(1.0 + 0.18 * jax.random.normal(key_of[5], (D,), jnp.float32), 0.1, 1.9)
    outer_gate = scatter_about(key_of[6], (D, SC), D ** -0.5, 0.125, ((0, 16), (1, 8)))
    inner_gate = scatter_about(key_of[7], (D, SC), D ** -0.5, 0.125, ((0, 16), (1, 8)))
    conv_input = scatter_about(key_of[8], (D, SC), D ** -0.5, 0.125, ((0, 16), (1, 8)))
    conv_taps = scatter_about(key_of[9], (KERNEL, SC), KERNEL ** -0.5, 3.5, ((1, 8),), jnp.float32)
    mixer_out = scatter_about(key_of[10], (SC, D), SC ** -0.5, 0.1875, ((0, 8), (1, 16)))
    gain_last = jnp.clip(1.0 + 0.18 * jax.random.normal(key_of[11], (D,), jnp.float32), 0.1, 1.9)
    gate_last = scatter_about(key_of[12], (D, FF), D ** -0.5, 0.125, ((0, 16), (1, 8)))
    up_last = scatter_about(key_of[13], (D, FF), D ** -0.5, 0.125, ((0, 16), (1, 8)))
    down_last = scatter_about(key_of[14], (FF, D), FF ** -0.5, 0.078125, ((0, 8), (1, 16)))
    return dict(tokens=tokens, gain_first=gain_first, gate_first=gate_first, up_first=up_first, down_first=down_first, gain_mixer=gain_mixer, outer_gate=outer_gate, inner_gate=inner_gate, conv_input=conv_input, conv_taps=conv_taps, mixer_out=mixer_out, gain_last=gain_last, gate_last=gate_last, up_last=up_last, down_last=down_last)


norm_eps = 1e-06

def rms_rows(residual, gain_vec):
    inverse = lax.rsqrt(lax.optimization_barrier(jnp.mean(residual * residual, axis=1, keepdims=True)) + norm_eps)
    return (residual * inverse * gain_vec).astype(jnp.bfloat16)

def blocked_sum(left_rows, right_rows):
    extent = left_rows.shape[1] // N_TP
    running = jnp.zeros((left_rows.shape[0], right_rows.shape[1]), jnp.float32)
    for block_id in range(N_TP):
        branch = jnp.dot(left_rows[:, block_id * extent:(block_id + 1) * extent], right_rows[block_id * extent:(block_id + 1) * extent], preferred_element_type=jnp.float32).astype(jnp.bfloat16)
        running = running + lax.optimization_barrier(branch).astype(jnp.float32)
    return running

def causal_mixing(gated, conv_taps):
    row_count, channels = gated.shape
    shaped = gated.reshape(row_count // SEQ_LEN, SEQ_LEN, channels)
    kernel = conv_taps.shape[0]
    padded = jnp.pad(shaped, ((0, 0), (kernel - 1, 0), (0, 0)))
    result = jnp.zeros_like(shaped)
    for offset in range(kernel):
        result = result + conv_taps[offset] * padded[:, offset:offset + SEQ_LEN]
    return result.reshape(row_count, channels)

def half_step(residual, gain_vec, gate_weight, up_weight, down_weight):
    normed = rms_rows(residual, gain_vec)
    gate_pre = jnp.dot(normed, gate_weight, preferred_element_type=jnp.float32)
    up_pre = jnp.dot(normed, up_weight, preferred_element_type=jnp.float32)
    hidden = (jax.nn.silu(gate_pre) * up_pre).astype(jnp.bfloat16)
    return residual + 0.5 * blocked_sum(hidden, down_weight)

def reference(tokens, gain_first, gate_first, up_first, down_first, gain_mixer, outer_gate, inner_gate, conv_input, conv_taps, mixer_out, gain_last, gate_last, up_last, down_last):
    residual = tokens.astype(jnp.float32)
    residual = half_step(residual, gain_first, gate_first, up_first, down_first)
    normed = rms_rows(residual, gain_mixer)
    outer_pre = jnp.dot(normed, outer_gate, preferred_element_type=jnp.float32)
    inner_pre = jnp.dot(normed, inner_gate, preferred_element_type=jnp.float32)
    value_pre = jnp.dot(normed, conv_input, preferred_element_type=jnp.float32)
    convolved = causal_mixing(inner_pre * value_pre, conv_taps)
    mixed_rows = (outer_pre * convolved).astype(jnp.bfloat16)
    residual = residual + blocked_sum(mixed_rows, mixer_out)
    residual = half_step(residual, gain_last, gate_last, up_last, down_last)
    return residual.astype(jnp.bfloat16)
```

```python
import functools

import jax
import jax.numpy as jnp
from jax import lax
from jax.experimental import pallas as pl
from jax.experimental.pallas import tpu as pltpu
from jax.sharding import PartitionSpec as P

SEQ_LEN = 64
EPS = 1e-06
MESH = pl.DeviceIdType.MESH
BF16 = jnp.bfloat16
F32 = jnp.float32

STREAMS = (("g1", 0), ("u1", 0), ("d1", 2), ("mx", 7), ("g2", 9), ("u2", 9), ("d2", 12))
PLAN = {
    ("g1", 0): ("ag_start0",),
    ("g1", 2): ("ag_pass0",),
    ("g1", 4): ("ag_far0",),
    ("g1", 6): ("norm0",),
    ("mx", 1): ("hidden1a",),
    ("d1", 7): ("hidden1b",),
    ("d1", 8): ("branch0",),
    ("g2", 2): ("pair0",),
    ("g2", 3): ("merge0",),
    ("mx", 6): ("finish0",),
    ("g2", 4): ("ag_start1",),
    ("u2", 4): ("ag_pass1",),
    ("g2", 5): ("ag_far1",),
    ("u2", 5): ("norm1",),
    ("d2", 3): ("mixer", "branch1"),
    ("u2", 7): ("pair1",),
    ("d2", 4): ("merge1",),
    ("g2", 8): ("finish1",),
    ("u2", 8): ("ag_start2",),
    ("d2", 5): ("ag_pass2",),
    ("d2", 6): ("ag_far2",),
    ("d2", 7): ("norm2",),
    ("d2", 8): ("hidden2a", "hidden2b", "branch2", "pair2", "merge2", "finish2"),
}


def own_part(rows, share, unit=16):
    return int(rows * share) // unit * unit


def layer(sizes, *refs):
    n_fs, n_tp, paired, splits = sizes
    (tokens, gain_first, gate_first, up_first, down_first, gain_mixer, outer_gate, inner_gate, conv_input, conv_taps,
     mixer_out, gain_last, gate_last, up_last, down_last, out,
     g1, u1, d1, mx, g2, u2, d2, raw, normed, hidden, mixed, res, acc, pair_out, pair_in, side_out, side_in,
     local_sem, z_send, z_recv, y_send, y_recv, x_send, x_recv) = refs
    rows, cols = tokens.shape
    half_rows = rows // 2
    half = n_fs // 2
    f = lax.axis_index("fs")
    t = lax.axis_index("tp")
    g = lax.axis_index("grp")
    n_x = n_tp // 2
    x, core = t // 2, t % 2
    par = g % 2
    depth = mx.shape[1] // 4

    up_fs, dn_fs = lax.rem(f + 1, n_fs), lax.rem(f + n_fs - 1, n_fs)
    ahead = lax.rem(x + 1, n_x) * 2 + core
    behind = lax.rem(x + n_x - 1, n_x) * 2 + core
    across = lax.rem(x + 2, n_x) * 2 + core
    partner = x * 2 + (1 - core)
    mate = g + 1 - 2 * par

    bufs = {"g1": g1, "u1": u1, "d1": d1, "mx": mx, "g2": g2, "u2": u2, "d2": d2}
    names = tuple(bufs)
    sources = {
        "g1": (gate_first,), "u1": (up_first,), "d1": (down_first,),
        "mx": (outer_gate, inner_gate, conv_input, mixer_out),
        "g2": (gate_last,), "u2": (up_last,), "d2": (down_last,),
    }

    loads = {}
    spare = 0
    own_tokens = pltpu.make_async_copy(tokens, raw.at[0, t], local_sem.at[spare])
    own_tokens.start()
    for name in names:
        loads[name] = []
        many = len(sources[name])
        for piece, source in enumerate(sources[name]):
            spare += 1
            place = bufs[name].at[f] if many == 1 else bufs[name].at[f, pl.ds(piece * depth, depth)]
            copy = pltpu.make_async_copy(source, place, local_sem.at[spare])
            copy.start()
            loads[name].append(copy)

    barrier = pltpu.get_barrier_semaphore()
    peers = [{"fs": up_fs}, {"fs": dn_fs}, {"tp": ahead}, {"tp": behind}, {"tp": partner}]
    if paired:
        peers.append({"grp": mate})
    for peer in peers:
        pl.semaphore_signal(barrier, inc=1, device_id=peer, device_id_type=MESH)
    pl.semaphore_wait(barrier, len(peers))

    def remote(source, target, send, recv, peer):
        return pltpu.make_async_remote_copy(
            src_ref=source, dst_ref=target, send_sem=send, recv_sem=recv, device_id=peer, device_id_type=MESH
        )

    in_flight = {}

    def send_slot(kind, count):
        queue = in_flight.setdefault(kind, [])
        if len(queue) == count:
            queue.pop(0).wait_send()
        position = in_flight.get((kind, "next"), 0)
        in_flight[(kind, "next")] = (position + 1) % count
        return position

    def ring_rows(name, direction, hop):
        alone, both = splits[name]
        length = alone + both
        start = par * alone
        if hop == half:
            first = (length // 2 + 15) // 16 * 16
            start, length = (start, first) if direction == 0 else (start + first, length - first)
        return pl.ds(pl.multiple_of(start, 16), length)

    def ring_copy(name, direction, hop, send=None):
        block = lax.rem(f + n_fs - (hop - 1), n_fs) if direction == 0 else lax.rem(f + hop - 1, n_fs)
        place = bufs[name].at[block, ring_rows(name, direction, hop)]
        send = 0 if send is None else send
        return remote(
            place, place, z_send.at[direction, send], z_recv.at[names.index(name), direction, hop - 1],
            {"fs": up_fs if direction == 0 else dn_fs},
        )

    def ring_start(name, direction, hop):
        slot = send_slot(("z", direction), z_send.shape[1])
        copy = ring_copy(name, direction, hop, slot)
        copy.start()
        in_flight[("z", direction)].append(copy)

    def hand_over(name, block):
        alone, both = splits[name]
        place = bufs[name].at[block, pl.ds(pl.multiple_of(par * (alone + both), 16), alone)]
        slot = send_slot("y", y_send.shape[0])
        copy = remote(place, place, y_send.at[slot], y_recv.at[names.index(name)], {"grp": mate})
        copy.start()
        in_flight["y"].append(copy)

    def ring_event(name, hop):
        if hop == 0:
            for copy in loads[name]:
                copy.wait()
            for direction in (0, 1):
                ring_start(name, direction, 1)
            return
        for direction in (0, 1):
            ring_copy(name, direction, hop).wait_recv()
            if hop < half:
                ring_start(name, direction, hop + 1)
        if paired:
            hand_over(name, lax.rem(f + n_fs - hop, n_fs))
            if hop < half:
                hand_over(name, lax.rem(f + hop, n_fs))

    def whole(name):
        if paired:
            alone = splits[name][0]
            view = bufs[name].at[pl.ds(0, n_fs - 1), pl.ds(0, alone)]
            pltpu.make_async_copy(view, view, y_recv.at[names.index(name)]).wait()

    x_flight = {}

    def x_start(number, phase, source, target, peer):
        if number in x_flight:
            x_flight[number].wait_send()
        copy = remote(source, target, x_send.at[number], x_recv.at[phase, number], peer)
        copy.start()
        x_flight[number] = copy

    def x_wait(number, phase, place):
        remote(place, place, x_send.at[number], x_recv.at[phase, number], {"tp": ahead}).wait_recv()

    low, high = pl.ds(0, half_rows), pl.ds(half_rows, half_rows)

    def ag_start(phase):
        if phase == 0:
            own_tokens.wait()
        own = raw.at[phase, t]
        x_start(0, phase, own, own, {"tp": ahead})
        x_start(1, phase, own, own, {"tp": behind})
        x_start(2, phase, own, own, {"tp": partner})

    def ag_pass(phase):
        prev, nxt = raw.at[phase, behind], raw.at[phase, ahead]
        x_wait(0, phase, prev)
        x_start(3, phase, raw.at[phase, behind, low], raw.at[phase, behind, low], {"tp": ahead})
        x_wait(1, phase, nxt)
        x_start(4, phase, raw.at[phase, ahead, high], raw.at[phase, ahead, high], {"tp": behind})
        x_start(5, phase, prev, prev, {"tp": partner})
        x_start(6, phase, nxt, nxt, {"tp": partner})

    def ag_far(phase):
        x_wait(3, phase, raw.at[phase, across, low])
        x_wait(4, phase, raw.at[phase, across, high])
        far = raw.at[phase, across]
        x_start(7, phase, far, far, {"tp": partner})

    def norm(phase, gain):
        for number in (2, 5, 6, 7):
            x_wait(number, phase, raw.at[phase, partner])
        step = 32

        def some(i, _):
            at = pl.ds(pl.multiple_of(i * step, step), step)
            parts = [raw[phase, j, at, :].astype(F32) for j in range(n_tp)]
            total = parts[0] * parts[0]
            for part in parts[1:]:
                total = total + part * part
            inverse = lax.rsqrt(jnp.sum(total, axis=1, keepdims=True) / (n_tp * cols) + EPS)
            for j, part in enumerate(parts):
                span = pl.ds(j * cols, cols)
                normed[at, span] = (part * inverse * gain[:, span]).astype(BF16)
            return 0

        lax.fori_loop(0, rows // step, some, 0)

    def hidden_tiles(gate, up, first, last):
        width = 128

        def tile(i, _):
            span = pl.ds(pl.multiple_of(i * width, width), width)
            k = gate.shape[0] * gate.shape[1]
            both = jnp.concatenate(
                [gate[:, :, span].reshape(k, width), up[:, :, span].reshape(k, width)], axis=1
            )
            pre = jnp.dot(normed[...], both, preferred_element_type=F32)
            gate_pre, up_pre = pre[:, :width], pre[:, width:]
            hidden[:, span] = (gate_pre / (1.0 + jnp.exp(-gate_pre)) * up_pre).astype(BF16)
            return 0

        lax.fori_loop(first, last, tile, 0)

    def mixer():
        whole("mx")
        k = n_fs * depth
        weight = lambda p: mx[:, p * depth:(p + 1) * depth, :].reshape(k, mx.shape[2])
        width = mx.shape[2]
        pair = jnp.dot(normed[...], jnp.concatenate([weight(1), weight(2)], axis=1), preferred_element_type=F32)
        gated = pair[:, :width] * pair[:, width:]
        place = lax.rem(lax.broadcasted_iota(jnp.int32, gated.shape, 0), SEQ_LEN)
        kernel = conv_taps.shape[0]
        convolved = gated * conv_taps[kernel - 1:kernel, :]
        for back in range(1, kernel):
            earlier = jnp.where(place >= back, pltpu.roll(gated, back, 0), 0.0)
            convolved = convolved + earlier * conv_taps[kernel - 1 - back:kernel - back, :]
        outer = jnp.dot(normed[...], weight(0), preferred_element_type=F32)
        mixed[...] = (outer * convolved).astype(BF16)

    def block_of(left, down, lead, owner):
        per = cols // down.shape[2]
        tiles = [down[owner * per + p][lead:, :] if lead else down[owner * per + p] for p in range(per)]
        return jnp.dot(left[...], jnp.concatenate(tiles, axis=1), preferred_element_type=F32)

    def branch(phase, left, name, lead):
        whole(name) if phase != 1 else None
        down = bufs[name]
        for j in range(n_x):
            if 8 + j in x_flight:
                x_flight.pop(8 + j).wait_send()

        def theirs(j, _):
            pair_out[j] = block_of(left, down, lead, lax.rem(x + j, n_x) * 2 + 1 - core).astype(BF16)
            return 0

        lax.fori_loop(0, n_x, theirs, 0)

        def pair_copy(j):
            return remote(pair_out.at[j], pair_in.at[phase, j], x_send.at[8 + j], x_recv.at[phase, 8 + j], {"tp": partner})

        def ours(j, _):
            pair_copy(j).start()
            acc[j] = block_of(left, down, lead, lax.rem(x + j, n_x) * 2 + core)
            return 0

        lax.fori_loop(0, n_x, ours, 0)
        for j in range(n_x):
            x_flight[8 + j] = pair_copy(j)

    def pair(phase):
        for j in (2, 1, 3, 0):
            x_wait(8 + j, phase, pair_in.at[phase, j])
        for number in range(12, 18):
            if number in x_flight:
                x_flight.pop(number).wait_send()
        for direction, keep in ((0, low), (1, high)):
            side_out[direction, 0] = (acc[2, keep, :] + pair_in[phase, 2, keep, :].astype(F32)).astype(BF16)
        for direction, near, keep in ((0, 1, high), (1, 3, low)):
            side_out[direction, 1] = (acc[near, keep, :] + pair_in[phase, near, keep, :].astype(F32)).astype(BF16)
        for near, keep in ((1, low), (3, high)):
            acc[near, keep, :] = acc[near, keep, :] + pair_in[phase, near, keep, :].astype(F32)
        acc[0] = acc[0] + pair_in[phase, 0].astype(F32)
        for order in (0, 1):
            for direction in (0, 1):
                side_start(phase, direction, order)

    def side_start(phase, direction, order):
        x_start(
            12 + 2 * order + direction, phase, side_out.at[direction, order], side_in.at[phase, direction, order],
            {"tp": ahead if direction == 0 else behind},
        )

    def side_wait(phase, direction, order):
        x_wait(12 + 2 * order + direction, phase, side_in.at[phase, direction, order])

    def merge(phase, factor):
        for direction, near, keep in ((0, 1, low), (1, 3, high)):
            side_wait(phase, direction, 0)
            side_out[direction, 2] = (acc[near, keep, :] + side_in[phase, direction, 0].astype(F32)).astype(BF16)
        res[...] = res[...] + factor * acc[0]
        for direction in (0, 1):
            side_start(phase, direction, 2)

    def finish(phase, factor):
        for order in (1, 2):
            for direction in (0, 1):
                side_wait(phase, direction, order)
        lo = side_in[phase, 0, 2].astype(F32) + side_in[phase, 1, 1].astype(F32)
        hi = side_in[phase, 0, 1].astype(F32) + side_in[phase, 1, 2].astype(F32)
        last = phase == 2
        for keep, extra in ((low, lo), (high, hi)):
            value = res[keep, :] + factor * extra
            if last:
                out[keep, :] = value.astype(BF16)
            else:
                res[keep, :] = value
                raw[phase + 1, t, keep, :] = value.astype(BF16)

    def hidden1a():
        whole("g1")
        whole("u1")
        hidden_tiles(g1, u1, 0, 3)

    def hidden2a():
        whole("g2")
        whole("u2")
        hidden_tiles(g2, u2, 0, 3)

    def norm0():
        norm(0, gain_first)
        res[...] = raw[0, t].astype(F32)

    tiles = g1.shape[2] // 128
    stages = {
        "ag_start0": lambda: ag_start(0), "ag_pass0": lambda: ag_pass(0), "ag_far0": lambda: ag_far(0),
        "norm0": norm0, "hidden1a": hidden1a, "hidden1b": lambda: hidden_tiles(g1, u1, 3, tiles),
        "branch0": lambda: branch(0, hidden, "d1", 0), "pair0": lambda: pair(0), "merge0": lambda: merge(0, 0.5),
        "finish0": lambda: finish(0, 0.5),
        "ag_start1": lambda: ag_start(1), "ag_pass1": lambda: ag_pass(1), "ag_far1": lambda: ag_far(1),
        "norm1": lambda: norm(1, gain_mixer), "mixer": mixer,
        "branch1": lambda: branch(1, mixed, "mx", 3 * depth), "pair1": lambda: pair(1), "merge1": lambda: merge(1, 1.0),
        "finish1": lambda: finish(1, 1.0),
        "ag_start2": lambda: ag_start(2), "ag_pass2": lambda: ag_pass(2), "ag_far2": lambda: ag_far(2),
        "norm2": lambda: norm(2, gain_last), "hidden2a": hidden2a, "hidden2b": lambda: hidden_tiles(g2, u2, 3, tiles),
        "branch2": lambda: branch(2, hidden, "d2", 0), "pair2": lambda: pair(2), "merge2": lambda: merge(2, 0.5),
        "finish2": lambda: finish(2, 0.5),
    }

    plan = plan_for(half)
    for event in ring_order(half):
        ring_event(*event)
        for stage in plan.get(event, ()):
            stages[stage]()

    for copy in list(x_flight.values()):
        copy.wait_send()
    for key, queue in in_flight.items():
        if isinstance(queue, list):
            for copy in queue:
                copy.wait_send()


def ring_order(half):
    events = []
    for step in range(max(first for _, first in STREAMS) + half + 1):
        for name, first in STREAMS:
            if 0 <= step - first <= half:
                events.append((name, step - first))
    return events


def plan_for(half):
    if half == 8:
        return PLAN
    last = ring_order(half)[-1]
    return {last: tuple(stage for stages in PLAN.values() for stage in stages)}


def fused_layer(n_fs, n_tp, n_grp, *args):
    tokens, gate, down, outer = args[0], args[2], args[4], args[6]
    rows, cols = tokens.shape
    paired = n_grp % 2 == 0
    n_x = n_tp // 2
    depth, hid = gate.shape
    chan = outer.shape[1]

    def split(length, share):
        alone = own_part(length, share) if paired else 0
        return alone, length - 2 * alone

    splits = {
        "g1": split(depth, 0.38), "u1": split(depth, 0.3), "d1": split(hid, 0.35), "mx": split(4 * depth, 0.35),
        "g2": split(depth, 0.38), "u2": split(depth, 0.3), "d2": split(hid, 0.35),
    }
    half = n_fs // 2
    wide = pltpu.VMEM((n_fs, depth, hid), BF16)
    tall = pltpu.VMEM((n_fs, hid, depth), BF16)
    gains = {1, 5, 11}
    args = [a.reshape(1, -1) if i in gains else a for i, a in enumerate(args)]
    vmem, anywhere = pl.BlockSpec(memory_space=pltpu.VMEM), pl.BlockSpec(memory_space=pl.ANY)
    in_vmem = gains | {9}
    return pl.pallas_call(
        functools.partial(layer, (n_fs, n_tp, paired, splits)),
        out_shape=jax.ShapeDtypeStruct((rows, cols), BF16),
        in_specs=[vmem if i in in_vmem else anywhere for i in range(len(args))],
        out_specs=vmem,
        scratch_shapes=[
            wide, wide, tall, pltpu.VMEM((n_fs, 4 * depth, chan), BF16), wide, wide, tall,
            pltpu.VMEM((3, n_tp, rows, cols), BF16),
            pltpu.VMEM((rows, n_tp * cols), BF16),
            pltpu.VMEM((rows, hid), BF16),
            pltpu.VMEM((rows, chan), BF16),
            pltpu.VMEM((rows, cols), F32),
            pltpu.VMEM((n_x, rows, cols), F32),
            pltpu.VMEM((n_x, rows, cols), BF16),
            pltpu.VMEM((3, n_x, rows, cols), BF16),
            pltpu.VMEM((2, 3, rows // 2, cols), BF16),
            pltpu.VMEM((3, 2, 3, rows // 2, cols), BF16),
            pltpu.SemaphoreType.DMA((11,)),
            pltpu.SemaphoreType.DMA((2, 8)),
            pltpu.SemaphoreType.DMA((7, 2, half)),
            pltpu.SemaphoreType.DMA((8,)),
            pltpu.SemaphoreType.DMA((7,)),
            pltpu.SemaphoreType.DMA((18,)),
            pltpu.SemaphoreType.DMA((3, 18)),
        ],
        compiler_params=pltpu.CompilerParams(
            collective_id=0, has_side_effects=True, vmem_limit_bytes=60 * 1024 * 1024
        ),
        name="fused_layer",
    )(*args)


def solution(mesh):
    in_specs = (
        P(("grp", "fs"), "tp"),
        P(),
        P("fs", "tp"),
        P("fs", "tp"),
        P("tp", "fs"),
        P(),
        P("fs", "tp"),
        P("fs", "tp"),
        P("fs", "tp"),
        P(None, "tp"),
        P("tp", "fs"),
        P(),
        P("fs", "tp"),
        P("fs", "tp"),
        P("tp", "fs"),
    )
    out_specs = P(("grp", "fs"), "tp")
    body = functools.partial(fused_layer, mesh.shape["fs"], mesh.shape["tp"], mesh.shape["grp"])
    return jax.shard_map(body, mesh=mesh, in_specs=in_specs, out_specs=out_specs, check_vma=False)
```

```python
import functools

import jax
import jax.numpy as jnp
from jax import lax
from jax.experimental import pallas as pl
from jax.experimental.pallas import tpu as pltpu
from jax.sharding import PartitionSpec as P

SEQ_LEN = 64
EPS = 1e-06
MESH = pl.DeviceIdType.MESH
BF16 = jnp.bfloat16
F32 = jnp.float32

EARLY = (
    (("u1", 0), 0, ("ag_start0",)),
    (("u1", 1), 0, ("ag_pass0", "ag_mid0")),
    (("u1", 2), 0, ("ag_far0",)),
    (("u1", 3), 0, ("norm0", "hidden1a")),
    (("u1", 4), 1, ("hidden1b",)),
    (("u1", 6), 1, ("hidden1c",)),
)
LATE = (
    (2, "hidden1d"), (3, "branch0"), (6, "merge0"), (8, "finish0"),
    (10, "ag_pass1"), (11, "ag_mid1"), (13, "ag_far1"), (14, "norm1"), (15, "mixer"), (17, "branch1"),
    (18, "merge1"), (20, "finish1"),
    (22, "ag_pass2"), (23, "ag_mid2"), (24, "ag_far2"), (25, "norm2"), (26, "hidden2a"), (27, "hidden2b"),
)
MIXED = (3, 3, 2, 2, 0)
LAST = ("hidden2c", "branch2", "merge2", "finish2")


def own_part(rows, share, unit=16):
    return int(rows * share) // unit * unit


def layer(sizes, *refs):
    n_fs, n_tp, paired, splits = sizes
    (tokens, gain_first, gate_first, up_first, down_first, gain_mixer, outer_gate, inner_gate, conv_input, conv_taps,
     mixer_out, gain_last, gate_last, up_last, down_last, out,
     g1, u1, d1, mx, g2, u2, d2, raw, normed, pre, hidden, mixed, res, acc, pair_out, pair_in, side_out, side_in,
     local_sem, z_send, z_recv, y_send, y_recv, x_send, x_recv) = refs
    rows, cols = tokens.shape
    half_rows = rows // 2
    half = n_fs // 2
    f = lax.axis_index("fs")
    t = lax.axis_index("tp")
    g = lax.axis_index("grp")
    n_x = n_tp // 2
    x, core = t // 2, t % 2
    par = g % 2
    depth = mx.shape[1] // 4
    per = cols // depth

    up_fs, dn_fs = lax.rem(f + 1, n_fs), lax.rem(f + n_fs - 1, n_fs)
    ahead = lax.rem(x + 1, n_x) * 2 + core
    behind = lax.rem(x + n_x - 1, n_x) * 2 + core
    across = lax.rem(x + 2, n_x) * 2 + core
    partner = x * 2 + (1 - core)
    mate = g + 1 - 2 * par

    bufs = {"g1": g1, "u1": u1, "d1": d1, "mx": mx, "g2": g2, "u2": u2, "d2": d2}
    names = tuple(bufs)
    sources = {
        "g1": (gate_first,), "u1": (up_first,), "d1": (down_first,),
        "mx": (outer_gate, inner_gate, conv_input, mixer_out),
        "g2": (gate_last,), "u2": (up_last,), "d2": (down_last,),
    }

    loads = {}
    spare = 0
    own_tokens = pltpu.make_async_copy(tokens, raw.at[0, t], local_sem.at[spare])
    own_tokens.start()
    for name in names:
        loads[name] = []
        many = len(sources[name])
        for piece, source in enumerate(sources[name]):
            spare += 1
            place = bufs[name].at[f] if many == 1 else bufs[name].at[f, pl.ds(piece * depth, depth)]
            copy = pltpu.make_async_copy(source, place, local_sem.at[spare])
            copy.start()
            loads[name].append(copy)

    barrier = pltpu.get_barrier_semaphore()
    peers = [{"fs": up_fs}, {"fs": dn_fs}, {"tp": ahead}, {"tp": behind}, {"tp": partner}]
    if paired:
        peers.append({"grp": mate})
    for peer in peers:
        pl.semaphore_signal(barrier, inc=1, device_id=peer, device_id_type=MESH)
    pl.semaphore_wait(barrier, len(peers))

    def remote(source, target, send, recv, peer):
        return pltpu.make_async_remote_copy(
            src_ref=source, dst_ref=target, send_sem=send, recv_sem=recv, device_id=peer, device_id_type=MESH
        )

    in_flight = {}

    def send_slot(kind, count):
        queue = in_flight.setdefault(kind, [])
        if len(queue) == count:
            queue.pop(0).wait_send()
        position = in_flight.get((kind, "next"), 0)
        in_flight[(kind, "next")] = (position + 1) % count
        return position

    def ring_rows(name, direction, hop):
        alone, both = splits[name]
        start, length = par * alone, alone + both
        if hop == half:
            first = (length // 2 + 15) // 16 * 16
            start, length = (start, first) if direction == 0 else (start + first, length - first)
        return pl.ds(pl.multiple_of(start, 16), length)

    def ring_copy(name, direction, hop, send=None):
        block = lax.rem(f + n_fs - (hop - 1), n_fs) if direction == 0 else lax.rem(f + hop - 1, n_fs)
        place = bufs[name].at[block, ring_rows(name, direction, hop)]
        send = 0 if send is None else send
        return remote(
            place, place, z_send.at[direction, send], z_recv.at[names.index(name), direction, hop - 1],
            {"fs": up_fs if direction == 0 else dn_fs},
        )

    def ring_start(name, direction, hop):
        slot = send_slot(("z", direction), z_send.shape[1])
        copy = ring_copy(name, direction, hop, slot)
        copy.start()
        in_flight[("z", direction)].append(copy)

    def hand_over(name, block, hop):
        alone, both = splits[name]
        place = bufs[name].at[block, pl.ds(pl.multiple_of(par * (alone + both), 16), alone)]
        slot = send_slot("y", y_send.shape[0])
        copy = remote(place, place, y_send.at[slot], y_recv.at[names.index(name), (hop - 1) // 2], {"grp": mate})
        copy.start()
        in_flight["y"].append(copy)

    def ring_event(name, hop):
        if hop == 0:
            for copy in loads[name]:
                copy.wait()
            for direction in (0, 1):
                ring_start(name, direction, 1)
            return
        for direction in (0, 1):
            ring_copy(name, direction, hop).wait_recv()
            if hop < half:
                ring_start(name, direction, hop + 1)
        if paired:
            hand_over(name, lax.rem(f + n_fs - hop, n_fs), hop)
            if hop < half:
                hand_over(name, lax.rem(f + hop, n_fs), hop)

    def whole(name, first=1, last=half):
        if paired:
            for stop in range(first + 1, last + 1, 2):
                view = bufs[name].at[pl.ds(0, 4 if stop < half else 3), pl.ds(0, splits[name][0])]
                pltpu.make_async_copy(view, view, y_recv.at[names.index(name), stop // 2 - 1]).wait()

    x_flight = {}

    def x_start(number, phase, source, target, peer):
        if number in x_flight:
            x_flight[number].wait_send()
        copy = remote(source, target, x_send.at[number], x_recv.at[phase % 2, number], peer)
        copy.start()
        x_flight[number] = copy

    def x_wait(number, phase, place):
        remote(place, place, x_send.at[number], x_recv.at[phase % 2, number], {"tp": ahead}).wait_recv()

    low, high = pl.ds(0, half_rows), pl.ds(half_rows, half_rows)

    def ag_start(phase):
        if phase == 0:
            own_tokens.wait()
        own, own_low, own_high = raw.at[phase, t], raw.at[phase, t, low], raw.at[phase, t, high]
        x_start(0, phase, own_low, own_low, {"tp": ahead})
        x_start(1, phase, own_high, own_high, {"tp": behind})
        x_start(2, phase, own_high, own_high, {"tp": ahead})
        x_start(3, phase, own_low, own_low, {"tp": behind})
        x_start(6, phase, own, own, {"tp": partner})

    def ag_pass(phase):
        prev, nxt = raw.at[phase, behind, low], raw.at[phase, ahead, high]
        x_wait(0, phase, prev)
        x_start(4, phase, prev, prev, {"tp": ahead})
        x_wait(1, phase, nxt)
        x_start(5, phase, nxt, nxt, {"tp": behind})

    def ag_mid(phase):
        prev, nxt = raw.at[phase, behind], raw.at[phase, ahead]
        x_wait(2, phase, raw.at[phase, behind, high])
        x_start(7, phase, prev, prev, {"tp": partner})
        x_wait(3, phase, raw.at[phase, ahead, low])
        x_start(8, phase, nxt, nxt, {"tp": partner})

    def ag_far(phase):
        x_wait(4, phase, raw.at[phase, across, low])
        x_wait(5, phase, raw.at[phase, across, high])
        far = raw.at[phase, across]
        x_start(9, phase, far, far, {"tp": partner})

    def norm(phase, gain):
        for number in (6, 7, 8, 9):
            x_wait(number, phase, raw.at[phase, partner])
        step = 32

        def some(i, _):
            at = pl.ds(pl.multiple_of(i * step, step), step)
            parts = [raw[phase, j, at, :].astype(F32) for j in range(n_tp)]
            total = parts[0] * parts[0]
            for part in parts[1:]:
                total = total + part * part
            inverse = lax.rsqrt(jnp.sum(total, axis=1, keepdims=True) / (n_tp * cols) + EPS)
            for j, part in enumerate(parts):
                value = (part * inverse * gain[:, pl.ds(j * cols, cols)]).astype(BF16)
                for p in range(per):
                    normed[j * per + p, at, :] = value[:, p * depth:(p + 1) * depth]
            return 0

        lax.fori_loop(0, rows // step, some, 0)

    def hidden_part(gate, up, nearest, farthest):
        width = 128
        shifts = []
        for hop in range(nearest, farthest + 1):
            shifts += [0] if hop == 0 else [half] if hop == half else [hop, n_fs - hop]
        blocks = [lax.rem(f + shift, n_fs) for shift in shifts]

        def tile(i, _):
            span = pl.ds(pl.multiple_of(i * width, width), width)
            left = jnp.concatenate([normed[b] for b in blocks], axis=1)
            right = jnp.concatenate(
                [jnp.concatenate([gate[b, :, span], up[b, :, span]], axis=1) for b in blocks], axis=0
            )
            product = jnp.dot(left, right, preferred_element_type=F32)
            if nearest:
                product = product + pre[i]
            if farthest < half:
                pre[i] = product
            else:
                gate_pre, up_pre = product[:, :width], product[:, width:]
                hidden[:, span] = (gate_pre / (1.0 + jnp.exp(-gate_pre)) * up_pre).astype(BF16)
            return 0

        lax.fori_loop(0, gate.shape[2] // width, tile, 0)

    def hidden_stage(gate, up, nearest, farthest):
        for name in (gate, up):
            whole(name, max(nearest, 1), farthest)
        hidden_part(bufs[gate], bufs[up], nearest, farthest)

    def mixer():
        whole("mx")
        k = n_fs * depth
        left = jnp.concatenate([normed[b] for b in range(n_fs)], axis=1)
        weight = lambda p: mx[:, p * depth:(p + 1) * depth, :].reshape(k, mx.shape[2])
        width = mx.shape[2]
        pair = jnp.dot(left, jnp.concatenate([weight(1), weight(2)], axis=1), preferred_element_type=F32)
        gated = pair[:, :width] * pair[:, width:]
        place = lax.rem(lax.broadcasted_iota(jnp.int32, gated.shape, 0), SEQ_LEN)
        kernel = conv_taps.shape[0]
        convolved = gated * conv_taps[kernel - 1:kernel, :]
        for back in range(1, kernel):
            earlier = jnp.where(place >= back, pltpu.roll(gated, back, 0), 0.0)
            convolved = convolved + earlier * conv_taps[kernel - 1 - back:kernel - back, :]
        outer = jnp.dot(left, weight(0), preferred_element_type=F32)
        mixed[...] = (outer * convolved).astype(BF16)

    def block_of(left, down, lead, owner):
        tiles = [down[owner * per + p][lead:, :] if lead else down[owner * per + p] for p in range(per)]
        return jnp.dot(left[...], jnp.concatenate(tiles, axis=1), preferred_element_type=F32)

    def branch(phase, left, name, lead, factor):
        if phase != 1:
            whole(name)
        down = bufs[name]
        for number in range(10, 20):
            if number in x_flight:
                x_flight.pop(number).wait_send()

        def block(j, side):
            return block_of(left, down, lead, lax.rem(x + j, n_x) * 2 + side)

        def pair_start(j):
            x_start(10 + j, phase, pair_out.at[j], pair_in.at[phase, j], {"tp": partner})

        def pair_sum(j, keep):
            return acc[j, keep, :] + pair_in[phase, j, keep, :].astype(F32)

        def theirs(j):
            pair_out[j] = block(j, 1 - core).astype(BF16)

        theirs(2)
        theirs(1)
        pair_start(2)
        acc[2] = block(2, core)
        pair_start(1)
        theirs(3)
        x_wait(12, phase, pair_in.at[phase, 2])
        for direction, keep in ((0, low), (1, high)):
            side_out[direction, 0] = pair_sum(2, keep).astype(BF16)
        acc[1] = block(1, core)
        pair_start(3)
        for direction in (0, 1):
            side_start(phase, direction, 0)
        theirs(0)
        acc[3] = block(3, core)
        pair_start(0)
        x_wait(11, phase, pair_in.at[phase, 1])
        x_wait(13, phase, pair_in.at[phase, 3])
        for direction, near, keep in ((0, 1, high), (1, 3, low)):
            side_out[direction, 1] = pair_sum(near, keep).astype(BF16)
        acc[0] = block(0, core)
        for direction in (0, 1):
            side_start(phase, direction, 1)
        for near, keep in ((1, low), (3, high)):
            acc[near, keep, :] = pair_sum(near, keep)
        x_wait(10, phase, pair_in.at[phase, 0])
        res[...] = res[...] + factor * (acc[0] + pair_in[phase, 0].astype(F32))

    def side_start(phase, direction, order):
        x_start(
            14 + 2 * order + direction, phase, side_out.at[direction, order], side_in.at[phase, direction, order],
            {"tp": ahead if direction == 0 else behind},
        )

    def side_wait(phase, direction, order):
        x_wait(14 + 2 * order + direction, phase, side_in.at[phase, direction, order])

    def merge(phase):
        for direction, near, keep in ((0, 1, low), (1, 3, high)):
            side_wait(phase, direction, 0)
            side_out[direction, 2] = (acc[near, keep, :] + side_in[phase, direction, 0].astype(F32)).astype(BF16)
        for direction in (0, 1):
            side_start(phase, direction, 2)

    def finish(phase, factor):
        for order in (1, 2):
            for direction in (0, 1):
                side_wait(phase, direction, order)
        lo = side_in[phase, 0, 2].astype(F32) + side_in[phase, 1, 1].astype(F32)
        hi = side_in[phase, 0, 1].astype(F32) + side_in[phase, 1, 2].astype(F32)
        target = out if phase == 2 else raw.at[phase + 1, t]
        for keep, extra in ((low, lo), (high, hi)):
            target[keep, :] = (res[keep, :] + factor * extra).astype(BF16)
        if phase < 2:
            for keep, extra in ((low, lo), (high, hi)):
                res[keep, :] = res[keep, :] + factor * extra
            ag_start(phase + 1)

    def norm0():
        norm(0, gain_first)
        res[...] = raw[0, t].astype(F32)

    stages = {
        "ag_start0": lambda: ag_start(0), "ag_pass0": lambda: ag_pass(0), "ag_mid0": lambda: ag_mid(0),
        "ag_far0": lambda: ag_far(0), "norm0": norm0,
        "hidden1a": lambda: hidden_stage("g1", "u1", 0, 2), "hidden1b": lambda: hidden_stage("g1", "u1", 3, 4),
        "hidden1c": lambda: hidden_stage("g1", "u1", 5, 6), "hidden1d": lambda: hidden_stage("g1", "u1", 7, half),
        "branch0": lambda: branch(0, hidden, "d1", 0, 0.5), "merge0": lambda: merge(0),
        "finish0": lambda: finish(0, 0.5),
        "ag_pass1": lambda: ag_pass(1), "ag_mid1": lambda: ag_mid(1),
        "ag_far1": lambda: ag_far(1),
        "norm1": lambda: norm(1, gain_mixer), "mixer": mixer,
        "branch1": lambda: branch(1, mixed, "mx", 3 * depth, 1.0), "merge1": lambda: merge(1),
        "finish1": lambda: finish(1, 1.0),
        "ag_pass2": lambda: ag_pass(2), "ag_mid2": lambda: ag_mid(2),
        "ag_far2": lambda: ag_far(2),
        "norm2": lambda: norm(2, gain_last), "hidden2a": lambda: hidden_stage("g2", "u2", 0, 4),
        "hidden2b": lambda: hidden_stage("g2", "u2", 5, 6), "hidden2c": lambda: hidden_stage("g2", "u2", 7, half),
        "branch2": lambda: branch(2, hidden, "d2", 0, 0.5), "merge2": lambda: merge(2),
        "finish2": lambda: finish(2, 0.5),
    }

    plan = plan_for(half)
    for event in ring_order(half):
        with jax.named_scope("ring_%s_%d" % event):
            ring_event(*event)
        for stage in plan.get(event, ()):
            with jax.named_scope(stage):
                stages[stage]()

    for copy in list(x_flight.values()):
        copy.wait_send()
    for key, queue in in_flight.items():
        if isinstance(queue, list):
            for copy in queue:
                copy.wait_send()


def ring_order(half):
    events = []
    lead = half // 2
    for hop in range(half + 1):
        events += [(name, hop) for name in ("d1", "g1", "u1")]
        if lead <= hop < half:
            events.append(("mx", hop - lead))
        if hop == half - 1:
            events += [(name, 0) for name in ("d2", "g2", "u2")]
    late = [(name, hop) for hop in range(1, half + 1) for name in ("d2", "g2", "u2")]
    for hop in range(half - lead, half + 1):
        events.append(("mx", hop))
        for _ in range(MIXED[hop - half + lead] if half == 8 else 2):
            events.append(late.pop(0))
    return events + late


def plan_for(half):
    events = ring_order(half)
    plan = {}
    if half != 8:
        every = [stage for _, _, stages in EARLY for stage in stages] + [stage for _, stage in LATE]
        plan[events[-1]] = tuple(every) + LAST
        return plan
    for anchor, offset, stages in EARLY:
        plan.setdefault(events[events.index(anchor) + offset], []).extend(stages)
    base = events.index(("u1", half))
    for offset, stage in LATE:
        plan.setdefault(events[base + offset], []).append(stage)
    plan.setdefault(events[-1], []).extend(LAST)
    return plan


def fused_layer(n_fs, n_tp, n_grp, *args):
    tokens, gate, down, outer = args[0], args[2], args[4], args[6]
    rows, cols = tokens.shape
    paired = n_grp % 2 == 0
    n_x = n_tp // 2
    depth, hid = gate.shape
    chan = outer.shape[1]

    def split(length, share):
        alone = own_part(length, share) if paired else 0
        return alone, length - 2 * alone

    splits = {
        "g1": split(depth, 0.38), "u1": split(depth, 0.3), "d1": split(hid, 0.35), "mx": split(4 * depth, 0.38),
        "g2": split(depth, 0.3), "u2": split(depth, 0.3), "d2": split(hid, 0.38),
    }
    half = n_fs // 2
    wide = pltpu.VMEM((n_fs, depth, hid), BF16)
    tall = pltpu.VMEM((n_fs, hid, depth), BF16)
    gains = {1, 5, 11}
    args = [a.reshape(1, -1) if i in gains else a for i, a in enumerate(args)]
    vmem, anywhere = pl.BlockSpec(memory_space=pltpu.VMEM), pl.BlockSpec(memory_space=pl.ANY)
    in_vmem = gains | {9}
    return pl.pallas_call(
        functools.partial(layer, (n_fs, n_tp, paired, splits)),
        out_shape=jax.ShapeDtypeStruct((rows, cols), BF16),
        in_specs=[vmem if i in in_vmem else anywhere for i in range(len(args))],
        out_specs=vmem,
        scratch_shapes=[
            wide, wide, tall, pltpu.VMEM((n_fs, 4 * depth, chan), BF16), wide, wide, tall,
            pltpu.VMEM((3, n_tp, rows, cols), BF16),
            pltpu.VMEM((n_fs, rows, depth), BF16),
            pltpu.VMEM((hid // 128, rows, 256), F32),
            pltpu.VMEM((rows, hid), BF16),
            pltpu.VMEM((rows, chan), BF16),
            pltpu.VMEM((rows, cols), F32),
            pltpu.VMEM((n_x, rows, cols), F32),
            pltpu.VMEM((n_x, rows, cols), BF16),
            pltpu.VMEM((3, n_x, rows, cols), BF16),
            pltpu.VMEM((2, 3, rows // 2, cols), BF16),
            pltpu.VMEM((3, 2, 3, rows // 2, cols), BF16),
            pltpu.SemaphoreType.DMA((11,)),
            pltpu.SemaphoreType.DMA((2, 4)),
            pltpu.SemaphoreType.DMA((7, 2, half)),
            pltpu.SemaphoreType.DMA((4,)),
            pltpu.SemaphoreType.DMA((7, half // 2)),
            pltpu.SemaphoreType.DMA((20,)),
            pltpu.SemaphoreType.DMA((2, 20)),
        ],
        compiler_params=pltpu.CompilerParams(
            collective_id=0, has_side_effects=True, vmem_limit_bytes=60 * 1024 * 1024
        ),
        name="fused_layer",
    )(*args)


def solution(mesh):
    in_specs = (
        P(("grp", "fs"), "tp"),
        P(),
        P("fs", "tp"),
        P("fs", "tp"),
        P("tp", "fs"),
        P(),
        P("fs", "tp"),
        P("fs", "tp"),
        P("fs", "tp"),
        P(None, "tp"),
        P("tp", "fs"),
        P(),
        P("fs", "tp"),
        P("fs", "tp"),
        P("tp", "fs"),
    )
    out_specs = P(("grp", "fs"), "tp")
    body = functools.partial(fused_layer, mesh.shape["fs"], mesh.shape["tp"], mesh.shape["grp"])
    return jax.shard_map(body, mesh=mesh, in_specs=in_specs, out_specs=out_specs, check_vma=False)
```

```python
import functools

import jax
import jax.numpy as jnp
from jax import lax
from jax.experimental import pallas as pl
from jax.experimental.pallas import tpu as pltpu
from jax.sharding import PartitionSpec as P

SEQ_LEN = 64
EPS = 1e-06
MESH = pl.DeviceIdType.MESH
BF16 = jnp.bfloat16
F32 = jnp.float32

EARLY = (
    (("u1", 0), 0, ("ag_start0",)),
    (("u1", 1), 0, ("ag_pass0", "ag_mid0")),
    (("u1", 2), 0, ("ag_far0",)),
    (("u1", 3), 0, ("norm0", "hidden1a")),
    (("u1", 4), 1, ("hidden1b",)),
    (("u1", 6), 1, ("hidden1c",)),
)
LATE = (
    (2, "hidden1d"), (3, "branch0"), (6, "merge0"), (8, "finish0"), (10, "ag_pass1"), (11, "ag_mid1"), (13, "ag_far1"), (14, "norm1"), (15, "mixer"), (16, "branch1"), (17, "merge1"), (19, "finish1"), (21, "ag_pass2"), (22, "ag_mid2"), (23, "ag_far2"), (24, "norm2"), (25, "hidden2a"), (26, "hidden2b"),
)
MIXED = (3, 3, 3, 0)
LAST = ("hidden2c", "branch2", "merge2", "finish2")


def own_part(rows, share, unit=16):
    return int(rows * share) // unit * unit


def layer(sizes, *refs):
    n_fs, n_tp, paired, splits = sizes
    (tokens, gain_first, gate_first, up_first, down_first, gain_mixer, outer_gate, inner_gate, conv_input, conv_taps,
     mixer_out, gain_last, gate_last, up_last, down_last, out,
     g1, u1, d1, mx, g2, u2, d2, raw, normed, pre, hidden, mixed, res, acc, pair_out, pair_in, side_out, side_in,
     local_sem, z_send, z_recv, y_send, y_recv, x_send, x_recv) = refs
    rows, cols = tokens.shape
    half_rows = rows // 2
    half = n_fs // 2
    f = lax.axis_index("fs")
    t = lax.axis_index("tp")
    g = lax.axis_index("grp")
    n_x = n_tp // 2
    x, core = t // 2, t % 2
    par = g % 2
    depth = mx.shape[1] // 4
    per = cols // depth

    up_fs, dn_fs = lax.rem(f + 1, n_fs), lax.rem(f + n_fs - 1, n_fs)
    ahead = lax.rem(x + 1, n_x) * 2 + core
    behind = lax.rem(x + n_x - 1, n_x) * 2 + core
    across = lax.rem(x + 2, n_x) * 2 + core
    partner = x * 2 + (1 - core)
    mate = g + 1 - 2 * par

    bufs = {"g1": g1, "u1": u1, "d1": d1, "mx": mx, "g2": g2, "u2": u2, "d2": d2}
    names = tuple(bufs)
    sources = {
        "g1": (gate_first,), "u1": (up_first,), "d1": (down_first,),
        "mx": (outer_gate, inner_gate, conv_input, mixer_out),
        "g2": (gate_last,), "u2": (up_last,), "d2": (down_last,),
    }

    loads = {}
    spare = 0
    own_tokens = pltpu.make_async_copy(tokens, raw.at[0, t], local_sem.at[spare])
    own_tokens.start()
    for name in names:
        loads[name] = []
        many = len(sources[name])
        for piece, source in enumerate(sources[name]):
            spare += 1
            place = bufs[name].at[f] if many == 1 else bufs[name].at[f, pl.ds(piece * depth, depth)]
            copy = pltpu.make_async_copy(source, place, local_sem.at[spare])
            copy.start()
            loads[name].append(copy)

    barrier = pltpu.get_barrier_semaphore()
    peers = [{"fs": up_fs}, {"fs": dn_fs}, {"tp": ahead}, {"tp": behind}, {"tp": partner}]
    if paired:
        peers.append({"grp": mate})
    for peer in peers:
        pl.semaphore_signal(barrier, inc=1, device_id=peer, device_id_type=MESH)
    pl.semaphore_wait(barrier, len(peers))

    def remote(source, target, send, recv, peer):
        return pltpu.make_async_remote_copy(
            src_ref=source, dst_ref=target, send_sem=send, recv_sem=recv, device_id=peer, device_id_type=MESH
        )

    in_flight = {}

    def send_slot(kind, count):
        queue = in_flight.setdefault(kind, [])
        if len(queue) == count:
            queue.pop(0).wait_send()
        position = in_flight.get((kind, "next"), 0)
        in_flight[(kind, "next")] = (position + 1) % count
        return position

    def ring_rows(name, direction, hop):
        alone, both = splits[name]
        start, length = par * alone, alone + both
        if hop == half:
            first = (length // 2 + 15) // 16 * 16
            start, length = (start, first) if direction == 0 else (start + first, length - first)
        return pl.ds(pl.multiple_of(start, 16), length)

    def ring_copy(name, direction, hop, send=None):
        block = lax.rem(f + n_fs - (hop - 1), n_fs) if direction == 0 else lax.rem(f + hop - 1, n_fs)
        place = bufs[name].at[block, ring_rows(name, direction, hop)]
        send = 0 if send is None else send
        return remote(
            place, place, z_send.at[direction, send], z_recv.at[names.index(name), direction, hop - 1],
            {"fs": up_fs if direction == 0 else dn_fs},
        )

    def ring_start(name, direction, hop):
        slot = send_slot(("z", direction), z_send.shape[1])
        copy = ring_copy(name, direction, hop, slot)
        copy.start()
        in_flight[("z", direction)].append(copy)

    def hand_over(name, block, hop):
        alone, both = splits[name]
        place = bufs[name].at[block, pl.ds(pl.multiple_of(par * (alone + both), 16), alone)]
        slot = send_slot("y", y_send.shape[0])
        copy = remote(place, place, y_send.at[slot], y_recv.at[names.index(name), (hop - 1) // 2], {"grp": mate})
        copy.start()
        in_flight["y"].append(copy)

    def ring_event(name, hop):
        if hop == 0:
            for copy in loads[name]:
                copy.wait()
            for direction in (0, 1):
                ring_start(name, direction, 1)
            return
        for direction in (0, 1):
            ring_copy(name, direction, hop).wait_recv()
            if hop < half:
                ring_start(name, direction, hop + 1)
        if paired:
            hand_over(name, lax.rem(f + n_fs - hop, n_fs), hop)
            if hop < half:
                hand_over(name, lax.rem(f + hop, n_fs), hop)

    def whole(name, first=1, last=half):
        if paired:
            for stop in range(first + 1, last + 1, 2):
                view = bufs[name].at[pl.ds(0, 4 if stop < half else 3), pl.ds(0, splits[name][0])]
                pltpu.make_async_copy(view, view, y_recv.at[names.index(name), stop // 2 - 1]).wait()

    x_flight = {}

    def x_start(number, phase, source, target, peer):
        if number in x_flight:
            x_flight[number].wait_send()
        copy = remote(source, target, x_send.at[number], x_recv.at[phase % 2, number], peer)
        copy.start()
        x_flight[number] = copy

    def x_wait(number, phase, place):
        remote(place, place, x_send.at[number], x_recv.at[phase % 2, number], {"tp": ahead}).wait_recv()

    low, high = pl.ds(0, half_rows), pl.ds(half_rows, half_rows)

    def ag_start(phase):
        if phase == 0:
            own_tokens.wait()
        own, own_low, own_high = raw.at[phase, t], raw.at[phase, t, low], raw.at[phase, t, high]
        x_start(0, phase, own_low, own_low, {"tp": ahead})
        x_start(1, phase, own_high, own_high, {"tp": behind})
        x_start(2, phase, own_high, own_high, {"tp": ahead})
        x_start(3, phase, own_low, own_low, {"tp": behind})
        x_start(6, phase, own, own, {"tp": partner})

    def ag_pass(phase):
        prev, nxt = raw.at[phase, behind, low], raw.at[phase, ahead, high]
        x_wait(0, phase, prev)
        x_start(4, phase, prev, prev, {"tp": ahead})
        x_wait(1, phase, nxt)
        x_start(5, phase, nxt, nxt, {"tp": behind})

    def ag_mid(phase):
        prev, nxt = raw.at[phase, behind], raw.at[phase, ahead]
        x_wait(2, phase, raw.at[phase, behind, high])
        x_start(7, phase, prev, prev, {"tp": partner})
        x_wait(3, phase, raw.at[phase, ahead, low])
        x_start(8, phase, nxt, nxt, {"tp": partner})

    def ag_far(phase):
        x_wait(4, phase, raw.at[phase, across, low])
        x_wait(5, phase, raw.at[phase, across, high])
        far = raw.at[phase, across]
        x_start(9, phase, far, far, {"tp": partner})

    def norm(phase, gain):
        for number in (6, 7, 8, 9):
            x_wait(number, phase, raw.at[phase, partner])
        step = 32

        def some(i, _):
            at = pl.ds(pl.multiple_of(i * step, step), step)
            parts = [raw[phase, j, at, :].astype(F32) for j in range(n_tp)]
            total = parts[0] * parts[0]
            for part in parts[1:]:
                total = total + part * part
            inverse = lax.rsqrt(jnp.sum(total, axis=1, keepdims=True) / (n_tp * cols) + EPS)
            for j, part in enumerate(parts):
                value = (part * inverse * gain[:, pl.ds(j * cols, cols)]).astype(BF16)
                for p in range(per):
                    normed[j * per + p, at, :] = value[:, p * depth:(p + 1) * depth]
            return 0

        lax.fori_loop(0, rows // step, some, 0)

    def hidden_part(gate, up, nearest, farthest):
        width = 128
        shifts = []
        for hop in range(nearest, farthest + 1):
            shifts += [0] if hop == 0 else [half] if hop == half else [hop, n_fs - hop]
        blocks = [lax.rem(f + shift, n_fs) for shift in shifts]

        def tile(i, _):
            span = pl.ds(pl.multiple_of(i * width, width), width)
            left = jnp.concatenate([normed[b] for b in blocks], axis=1)
            right = jnp.concatenate(
                [jnp.concatenate([gate[b, :, span], up[b, :, span]], axis=1) for b in blocks], axis=0
            )
            product = jnp.dot(left, right, preferred_element_type=F32)
            if nearest:
                product = product + pre[i]
            if farthest < half:
                pre[i] = product
            else:
                gate_pre, up_pre = product[:, :width], product[:, width:]
                hidden[:, span] = (gate_pre / (1.0 + jnp.exp(-gate_pre)) * up_pre).astype(BF16)
            return 0

        lax.fori_loop(0, gate.shape[2] // width, tile, 0)

    def hidden_stage(gate, up, nearest, farthest):
        for name in (gate, up):
            whole(name, max(nearest, 1), farthest)
        hidden_part(bufs[gate], bufs[up], nearest, farthest)

    def mixer():
        whole("mx")
        k = n_fs * depth
        left = jnp.concatenate([normed[b] for b in range(n_fs)], axis=1)
        weight = lambda p: mx[:, p * depth:(p + 1) * depth, :].reshape(k, mx.shape[2])
        width = mx.shape[2]
        pair = jnp.dot(left, jnp.concatenate([weight(1), weight(2)], axis=1), preferred_element_type=F32)
        gated = pair[:, :width] * pair[:, width:]
        place = lax.rem(lax.broadcasted_iota(jnp.int32, gated.shape, 0), SEQ_LEN)
        kernel = conv_taps.shape[0]
        convolved = gated * conv_taps[kernel - 1:kernel, :]
        for back in range(1, kernel):
            earlier = jnp.where(place >= back, pltpu.roll(gated, back, 0), 0.0)
            convolved = convolved + earlier * conv_taps[kernel - 1 - back:kernel - back, :]
        outer = jnp.dot(left, weight(0), preferred_element_type=F32)
        mixed[...] = (outer * convolved).astype(BF16)

    def block_of(left, down, lead, owner):
        tiles = [down[owner * per + p][lead:, :] if lead else down[owner * per + p] for p in range(per)]
        return jnp.dot(left[...], jnp.concatenate(tiles, axis=1), preferred_element_type=F32)

    def branch(phase, left, name, lead, factor):
        if phase != 1:
            whole(name)
        down = bufs[name]
        for number in range(10, 20):
            if number in x_flight:
                x_flight.pop(number).wait_send()

        def block(j, side):
            return block_of(left, down, lead, lax.rem(x + j, n_x) * 2 + side)

        def pair_start(j):
            x_start(10 + j, phase, pair_out.at[j], pair_in.at[phase, j], {"tp": partner})

        def pair_sum(j, keep):
            return acc[j, keep, :] + pair_in[phase, j, keep, :].astype(F32)

        def theirs(j):
            pair_out[j] = block(j, 1 - core).astype(BF16)

        theirs(2)
        theirs(1)
        pair_start(2)
        acc[2] = block(2, core)
        pair_start(1)
        theirs(3)
        x_wait(12, phase, pair_in.at[phase, 2])
        for direction, keep in ((0, low), (1, high)):
            side_out[direction, 0] = pair_sum(2, keep).astype(BF16)
        acc[1] = block(1, core)
        pair_start(3)
        for direction in (0, 1):
            side_start(phase, direction, 0)
        theirs(0)
        acc[3] = block(3, core)
        pair_start(0)
        x_wait(11, phase, pair_in.at[phase, 1])
        x_wait(13, phase, pair_in.at[phase, 3])
        for direction, near, keep in ((0, 1, high), (1, 3, low)):
            side_out[direction, 1] = pair_sum(near, keep).astype(BF16)
        acc[0] = block(0, core)
        for direction in (0, 1):
            side_start(phase, direction, 1)
        for near, keep in ((1, low), (3, high)):
            acc[near, keep, :] = pair_sum(near, keep)
        x_wait(10, phase, pair_in.at[phase, 0])
        res[...] = res[...] + factor * (acc[0] + pair_in[phase, 0].astype(F32))

    def side_start(phase, direction, order):
        x_start(
            14 + 2 * order + direction, phase, side_out.at[direction, order], side_in.at[phase, direction, order],
            {"tp": ahead if direction == 0 else behind},
        )

    def side_wait(phase, direction, order):
        x_wait(14 + 2 * order + direction, phase, side_in.at[phase, direction, order])

    def merge(phase):
        for direction, near, keep in ((0, 1, low), (1, 3, high)):
            side_wait(phase, direction, 0)
            side_out[direction, 2] = (acc[near, keep, :] + side_in[phase, direction, 0].astype(F32)).astype(BF16)
        for direction in (0, 1):
            side_start(phase, direction, 2)

    def finish(phase, factor):
        for order in (1, 2):
            for direction in (0, 1):
                side_wait(phase, direction, order)
        lo = side_in[phase, 0, 2].astype(F32) + side_in[phase, 1, 1].astype(F32)
        hi = side_in[phase, 0, 1].astype(F32) + side_in[phase, 1, 2].astype(F32)
        target = out if phase == 2 else raw.at[phase + 1, t]
        for keep, extra in ((low, lo), (high, hi)):
            target[keep, :] = (res[keep, :] + factor * extra).astype(BF16)
        if phase < 2:
            for keep, extra in ((low, lo), (high, hi)):
                res[keep, :] = res[keep, :] + factor * extra
            ag_start(phase + 1)

    def norm0():
        norm(0, gain_first)
        res[...] = raw[0, t].astype(F32)

    stages = {
        "ag_start0": lambda: ag_start(0), "ag_pass0": lambda: ag_pass(0), "ag_mid0": lambda: ag_mid(0),
        "ag_far0": lambda: ag_far(0), "norm0": norm0,
        "hidden1a": lambda: hidden_stage("g1", "u1", 0, 2), "hidden1b": lambda: hidden_stage("g1", "u1", 3, 4),
        "hidden1c": lambda: hidden_stage("g1", "u1", 5, 6), "hidden1d": lambda: hidden_stage("g1", "u1", 7, half),
        "branch0": lambda: branch(0, hidden, "d1", 0, 0.5), "merge0": lambda: merge(0),
        "finish0": lambda: finish(0, 0.5),
        "ag_pass1": lambda: ag_pass(1), "ag_mid1": lambda: ag_mid(1),
        "ag_far1": lambda: ag_far(1),
        "norm1": lambda: norm(1, gain_mixer), "mixer": mixer,
        "branch1": lambda: branch(1, mixed, "mx", 3 * depth, 1.0), "merge1": lambda: merge(1),
        "finish1": lambda: finish(1, 1.0),
        "ag_pass2": lambda: ag_pass(2), "ag_mid2": lambda: ag_mid(2),
        "ag_far2": lambda: ag_far(2),
        "norm2": lambda: norm(2, gain_last), "hidden2a": lambda: hidden_stage("g2", "u2", 0, 4),
        "hidden2b": lambda: hidden_stage("g2", "u2", 5, 6), "hidden2c": lambda: hidden_stage("g2", "u2", 7, half),
        "branch2": lambda: branch(2, hidden, "d2", 0, 0.5), "merge2": lambda: merge(2),
        "finish2": lambda: finish(2, 0.5),
    }

    plan = plan_for(half)
    for event in ring_order(half):
        with jax.named_scope("ring_%s_%d" % event):
            ring_event(*event)
        for stage in plan.get(event, ()):
            with jax.named_scope(stage):
                stages[stage]()

    for copy in list(x_flight.values()):
        copy.wait_send()
    for key, queue in in_flight.items():
        if isinstance(queue, list):
            for copy in queue:
                copy.wait_send()


def ring_order(half):
    events = []
    lead = half // 2 - 1
    for hop in range(half + 1):
        events += [(name, hop) for name in ("d1", "g1", "u1")]
        if lead <= hop < half:
            events.append(("mx", hop - lead))
        if hop == half - 1:
            events += [(name, 0) for name in ("g2", "u2", "d2")]
    late = [(name, hop) for hop in range(1, half + 1) for name in ("g2", "u2", "d2")]
    for hop in range(half - lead, half + 1):
        events.append(("mx", hop))
        for _ in range(MIXED[hop - half + lead] if half == 8 else 2):
            events.append(late.pop(0))
    return events + late


def plan_for(half):
    events = ring_order(half)
    plan = {}
    if half != 8:
        every = [stage for _, _, stages in EARLY for stage in stages] + [stage for _, stage in LATE]
        plan[events[-1]] = tuple(every) + LAST
        return plan
    for anchor, offset, stages in EARLY:
        plan.setdefault(events[events.index(anchor) + offset], []).extend(stages)
    base = events.index(("u1", half))
    for offset, stage in LATE:
        plan.setdefault(events[base + offset], []).append(stage)
    plan.setdefault(events[-1], []).extend(LAST)
    return plan


def fused_layer(n_fs, n_tp, n_grp, *args):
    tokens, gate, down, outer = args[0], args[2], args[4], args[6]
    rows, cols = tokens.shape
    paired = n_grp % 2 == 0
    n_x = n_tp // 2
    depth, hid = gate.shape
    chan = outer.shape[1]

    def split(length, share):
        alone = own_part(length, share) if paired else 0
        return alone, length - 2 * alone

    splits = {
        "g1": split(depth, 0.38), "u1": split(depth, 0.3), "d1": split(hid, 0.35), "mx": split(4 * depth, 0.38),
        "g2": split(depth, 0.3), "u2": split(depth, 0.3), "d2": split(hid, 0.38),
    }
    half = n_fs // 2
    wide = pltpu.VMEM((n_fs, depth, hid), BF16)
    tall = pltpu.VMEM((n_fs, hid, depth), BF16)
    gains = {1, 5, 11}
    args = [a.reshape(1, -1) if i in gains else a for i, a in enumerate(args)]
    vmem, anywhere = pl.BlockSpec(memory_space=pltpu.VMEM), pl.BlockSpec(memory_space=pl.ANY)
    in_vmem = gains | {9}
    return pl.pallas_call(
        functools.partial(layer, (n_fs, n_tp, paired, splits)),
        out_shape=jax.ShapeDtypeStruct((rows, cols), BF16),
        in_specs=[vmem if i in in_vmem else anywhere for i in range(len(args))],
        out_specs=vmem,
        scratch_shapes=[
            wide, wide, tall, pltpu.VMEM((n_fs, 4 * depth, chan), BF16), wide, wide, tall,
            pltpu.VMEM((3, n_tp, rows, cols), BF16),
            pltpu.VMEM((n_fs, rows, depth), BF16),
            pltpu.VMEM((hid // 128, rows, 256), F32),
            pltpu.VMEM((rows, hid), BF16),
            pltpu.VMEM((rows, chan), BF16),
            pltpu.VMEM((rows, cols), F32),
            pltpu.VMEM((n_x, rows, cols), F32),
            pltpu.VMEM((n_x, rows, cols), BF16),
            pltpu.VMEM((3, n_x, rows, cols), BF16),
            pltpu.VMEM((2, 3, rows // 2, cols), BF16),
            pltpu.VMEM((3, 2, 3, rows // 2, cols), BF16),
            pltpu.SemaphoreType.DMA((11,)),
            pltpu.SemaphoreType.DMA((2, 4)),
            pltpu.SemaphoreType.DMA((7, 2, half)),
            pltpu.SemaphoreType.DMA((4,)),
            pltpu.SemaphoreType.DMA((7, half // 2)),
            pltpu.SemaphoreType.DMA((20,)),
            pltpu.SemaphoreType.DMA((2, 20)),
        ],
        compiler_params=pltpu.CompilerParams(
            collective_id=0, has_side_effects=True, vmem_limit_bytes=60 * 1024 * 1024
        ),
        name="fused_layer",
    )(*args)


def solution(mesh):
    in_specs = (
        P(("grp", "fs"), "tp"),
        P(),
        P("fs", "tp"),
        P("fs", "tp"),
        P("tp", "fs"),
        P(),
        P("fs", "tp"),
        P("fs", "tp"),
        P("fs", "tp"),
        P(None, "tp"),
        P("tp", "fs"),
        P(),
        P("fs", "tp"),
        P("fs", "tp"),
        P("tp", "fs"),
    )
    out_specs = P(("grp", "fs"), "tp")
    body = functools.partial(fused_layer, mesh.shape["fs"], mesh.shape["tp"], mesh.shape["grp"])
    return jax.shard_map(body, mesh=mesh, in_specs=in_specs, out_specs=out_specs, check_vma=False)
```

```python
import functools

import jax
import jax.numpy as jnp
from jax import lax
from jax.experimental import pallas as pl
from jax.experimental.pallas import tpu as pltpu
from jax.sharding import PartitionSpec as P

SEQ_LEN = 64
EPS = 1e-06
MESH = pl.DeviceIdType.MESH
BF16 = jnp.bfloat16
F32 = jnp.float32

EARLY = (
    (("u1", 0), 0, ("ag_start0",)),
    (("u1", 1), 0, ("ag_pass0", "ag_mid0")),
    (("u1", 2), 0, ("ag_far0",)),
    (("u1", 3), 0, ("norm0", "hidden1a")),
    (("u1", 4), 1, ("hidden1b",)),
    (("u1", 6), 1, ("hidden1c",)),
)
LATE = (
    (2, "hidden1d"), (3, "branch0"), (6, "merge0"), (8, "finish0"), (10, "ag_pass1"), (11, "ag_mid1"), (13, "ag_far1"), (14, "norm1"), (15, "mixer"), (16, "branch1"), (17, "merge1"), (19, "finish1"), (22, "ag_pass2"), (22, "ag_mid2"), (23, "ag_far2"), (24, "norm2"), (25, "hidden2a"),
)
MIXED = (3, 3, 3, 0)
LAST = ("hidden2c", "branch2", "merge2", "finish2")


def own_part(rows, share, unit=16):
    return int(rows * share) // unit * unit


def layer(sizes, *refs):
    n_fs, n_tp, paired, splits = sizes
    (tokens, gain_first, gate_first, up_first, down_first, gain_mixer, outer_gate, inner_gate, conv_input, conv_taps,
     mixer_out, gain_last, gate_last, up_last, down_last, out,
     g1, u1, d1, mx, g2, u2, d2, raw, normed, pre, hidden, mixed, res, acc, pair_out, pair_in, side_out, side_in,
     local_sem, z_send, z_recv, y_send, y_recv, x_send, x_recv) = refs
    rows, cols = tokens.shape
    half_rows = rows // 2
    half = n_fs // 2
    f = lax.axis_index("fs")
    t = lax.axis_index("tp")
    g = lax.axis_index("grp")
    n_x = n_tp // 2
    x, core = t // 2, t % 2
    par = g % 2
    depth = mx.shape[1] // 4
    per = cols // depth

    up_fs, dn_fs = lax.rem(f + 1, n_fs), lax.rem(f + n_fs - 1, n_fs)
    ahead = lax.rem(x + 1, n_x) * 2 + core
    behind = lax.rem(x + n_x - 1, n_x) * 2 + core
    across = lax.rem(x + 2, n_x) * 2 + core
    partner = x * 2 + (1 - core)
    mate = g + 1 - 2 * par

    bufs = {"g1": g1, "u1": u1, "d1": d1, "mx": mx, "g2": g2, "u2": u2, "d2": d2}
    names = tuple(bufs)
    sources = {
        "g1": (gate_first,), "u1": (up_first,), "d1": (down_first,),
        "mx": (outer_gate, inner_gate, conv_input, mixer_out),
        "g2": (gate_last,), "u2": (up_last,), "d2": (down_last,),
    }

    loads = {}
    spare = 0
    own_tokens = pltpu.make_async_copy(tokens, raw.at[0, t], local_sem.at[spare])
    own_tokens.start()
    for name in names:
        loads[name] = []
        many = len(sources[name])
        for piece, source in enumerate(sources[name]):
            spare += 1
            place = bufs[name].at[f] if many == 1 else bufs[name].at[f, pl.ds(piece * depth, depth)]
            copy = pltpu.make_async_copy(source, place, local_sem.at[spare])
            copy.start()
            loads[name].append(copy)

    barrier = pltpu.get_barrier_semaphore()
    peers = [{"fs": up_fs}, {"fs": dn_fs}, {"tp": ahead}, {"tp": behind}, {"tp": partner}]
    if paired:
        peers.append({"grp": mate})
    for peer in peers:
        pl.semaphore_signal(barrier, inc=1, device_id=peer, device_id_type=MESH)
    pl.semaphore_wait(barrier, len(peers))

    def remote(source, target, send, recv, peer):
        return pltpu.make_async_remote_copy(
            src_ref=source, dst_ref=target, send_sem=send, recv_sem=recv, device_id=peer, device_id_type=MESH
        )

    in_flight = {}

    def send_slot(kind, count):
        queue = in_flight.setdefault(kind, [])
        if len(queue) == count:
            queue.pop(0).wait_send()
        position = in_flight.get((kind, "next"), 0)
        in_flight[(kind, "next")] = (position + 1) % count
        return position

    def ring_rows(name, direction, hop):
        alone, both = splits[name]
        start, length = par * alone, alone + both
        if hop == half:
            first = (length // 2 + 15) // 16 * 16
            start, length = (start, first) if direction == 0 else (start + first, length - first)
        return pl.ds(pl.multiple_of(start, 16), length)

    def ring_copy(name, direction, hop, send=None):
        block = lax.rem(f + n_fs - (hop - 1), n_fs) if direction == 0 else lax.rem(f + hop - 1, n_fs)
        place = bufs[name].at[block, ring_rows(name, direction, hop)]
        send = 0 if send is None else send
        return remote(
            place, place, z_send.at[direction, send], z_recv.at[names.index(name), direction, hop - 1],
            {"fs": up_fs if direction == 0 else dn_fs},
        )

    def ring_start(name, direction, hop):
        slot = send_slot(("z", direction), z_send.shape[1])
        copy = ring_copy(name, direction, hop, slot)
        copy.start()
        in_flight[("z", direction)].append(copy)

    def hand_over(name, block, hop):
        alone, both = splits[name]
        place = bufs[name].at[block, pl.ds(pl.multiple_of(par * (alone + both), 16), alone)]
        slot = send_slot("y", y_send.shape[0])
        copy = remote(place, place, y_send.at[slot], y_recv.at[names.index(name), (hop - 1) // 2], {"grp": mate})
        copy.start()
        in_flight["y"].append(copy)

    def ring_event(name, hop):
        if hop == 0:
            for copy in loads[name]:
                copy.wait()
            for direction in (0, 1):
                ring_start(name, direction, 1)
            return
        for direction in (0, 1):
            ring_copy(name, direction, hop).wait_recv()
            if hop < half:
                ring_start(name, direction, hop + 1)
        if paired:
            hand_over(name, lax.rem(f + n_fs - hop, n_fs), hop)
            if hop < half:
                hand_over(name, lax.rem(f + hop, n_fs), hop)

    def whole(name, first=1, last=half):
        if paired:
            for stop in range(first + 1, last + 1, 2):
                view = bufs[name].at[pl.ds(0, 4 if stop < half else 3), pl.ds(0, splits[name][0])]
                pltpu.make_async_copy(view, view, y_recv.at[names.index(name), stop // 2 - 1]).wait()

    x_flight = {}

    def x_start(number, phase, source, target, peer):
        if number in x_flight:
            x_flight[number].wait_send()
        copy = remote(source, target, x_send.at[number], x_recv.at[phase % 2, number], peer)
        copy.start()
        x_flight[number] = copy

    def x_wait(number, phase, place):
        remote(place, place, x_send.at[number], x_recv.at[phase % 2, number], {"tp": ahead}).wait_recv()

    low, high = pl.ds(0, half_rows), pl.ds(half_rows, half_rows)

    def ag_start(phase):
        if phase == 0:
            own_tokens.wait()
        own, own_low, own_high = raw.at[phase, t], raw.at[phase, t, low], raw.at[phase, t, high]
        x_start(0, phase, own_low, own_low, {"tp": ahead})
        x_start(1, phase, own_high, own_high, {"tp": behind})
        x_start(2, phase, own_high, own_high, {"tp": ahead})
        x_start(3, phase, own_low, own_low, {"tp": behind})
        x_start(6, phase, own, own, {"tp": partner})

    def ag_pass(phase):
        prev, nxt = raw.at[phase, behind, low], raw.at[phase, ahead, high]
        x_wait(0, phase, prev)
        x_start(4, phase, prev, prev, {"tp": ahead})
        x_wait(1, phase, nxt)
        x_start(5, phase, nxt, nxt, {"tp": behind})

    def ag_mid(phase):
        prev, nxt = raw.at[phase, behind], raw.at[phase, ahead]
        x_wait(2, phase, raw.at[phase, behind, high])
        x_start(7, phase, prev, prev, {"tp": partner})
        x_wait(3, phase, raw.at[phase, ahead, low])
        x_start(8, phase, nxt, nxt, {"tp": partner})

    def ag_far(phase):
        x_wait(4, phase, raw.at[phase, across, low])
        x_wait(5, phase, raw.at[phase, across, high])
        far = raw.at[phase, across]
        x_start(9, phase, far, far, {"tp": partner})

    def norm(phase, gain):
        for number in (6, 7, 8, 9):
            x_wait(number, phase, raw.at[phase, partner])
        step = 32

        def some(i, _):
            at = pl.ds(pl.multiple_of(i * step, step), step)
            parts = [raw[phase, j, at, :].astype(F32) for j in range(n_tp)]
            total = parts[0] * parts[0]
            for part in parts[1:]:
                total = total + part * part
            inverse = lax.rsqrt(jnp.sum(total, axis=1, keepdims=True) / (n_tp * cols) + EPS)
            for j, part in enumerate(parts):
                value = (part * inverse * gain[:, pl.ds(j * cols, cols)]).astype(BF16)
                for p in range(per):
                    normed[j * per + p, at, :] = value[:, p * depth:(p + 1) * depth]
            return 0

        lax.fori_loop(0, rows // step, some, 0)

    def hidden_part(gate, up, nearest, farthest):
        width = 128
        shifts = []
        for hop in range(nearest, farthest + 1):
            shifts += [0] if hop == 0 else [half] if hop == half else [hop, n_fs - hop]
        blocks = [lax.rem(f + shift, n_fs) for shift in shifts]

        def tile(i, _):
            span = pl.ds(pl.multiple_of(i * width, width), width)
            left = jnp.concatenate([normed[b] for b in blocks], axis=1)
            right = jnp.concatenate(
                [jnp.concatenate([gate[b, :, span], up[b, :, span]], axis=1) for b in blocks], axis=0
            )
            product = jnp.dot(left, right, preferred_element_type=F32)
            if nearest:
                product = product + pre[i]
            if farthest < half:
                pre[i] = product
            else:
                gate_pre, up_pre = product[:, :width], product[:, width:]
                hidden[:, span] = (gate_pre / (1.0 + jnp.exp(-gate_pre)) * up_pre).astype(BF16)
            return 0

        lax.fori_loop(0, gate.shape[2] // width, tile, 0)

    def hidden_stage(gate, up, nearest, farthest):
        for name in (gate, up):
            whole(name, max(nearest, 1), farthest)
        hidden_part(bufs[gate], bufs[up], nearest, farthest)

    def mixer():
        whole("mx")
        k = n_fs * depth
        left = jnp.concatenate([normed[b] for b in range(n_fs)], axis=1)
        weight = lambda p: mx[:, p * depth:(p + 1) * depth, :].reshape(k, mx.shape[2])
        width = mx.shape[2]
        pair = jnp.dot(left, jnp.concatenate([weight(1), weight(2)], axis=1), preferred_element_type=F32)
        gated = pair[:, :width] * pair[:, width:]
        place = lax.rem(lax.broadcasted_iota(jnp.int32, gated.shape, 0), SEQ_LEN)
        kernel = conv_taps.shape[0]
        convolved = gated * conv_taps[kernel - 1:kernel, :]
        for back in range(1, kernel):
            earlier = jnp.where(place >= back, pltpu.roll(gated, back, 0), 0.0)
            convolved = convolved + earlier * conv_taps[kernel - 1 - back:kernel - back, :]
        outer = jnp.dot(left, weight(0), preferred_element_type=F32)
        mixed[...] = (outer * convolved).astype(BF16)

    def block_of(left, down, lead, owner):
        tiles = [down[owner * per + p][lead:, :] if lead else down[owner * per + p] for p in range(per)]
        return jnp.dot(left[...], jnp.concatenate(tiles, axis=1), preferred_element_type=F32)

    def branch(phase, left, name, lead, factor):
        if phase != 1:
            whole(name)
        down = bufs[name]
        for number in range(10, 20):
            if number in x_flight:
                x_flight.pop(number).wait_send()

        def block(j, side):
            return block_of(left, down, lead, lax.rem(x + j, n_x) * 2 + side)

        def pair_start(j):
            x_start(10 + j, phase, pair_out.at[j], pair_in.at[phase, j], {"tp": partner})

        def pair_sum(j, keep):
            return acc[j, keep, :] + pair_in[phase, j, keep, :].astype(F32)

        def theirs(j):
            pair_out[j] = block(j, 1 - core).astype(BF16)

        theirs(2)
        theirs(1)
        pair_start(2)
        acc[2] = block(2, core)
        pair_start(1)
        theirs(3)
        x_wait(12, phase, pair_in.at[phase, 2])
        for direction, keep in ((0, low), (1, high)):
            side_out[direction, 0] = pair_sum(2, keep).astype(BF16)
        acc[1] = block(1, core)
        pair_start(3)
        for direction in (0, 1):
            side_start(phase, direction, 0)
        theirs(0)
        acc[3] = block(3, core)
        pair_start(0)
        x_wait(11, phase, pair_in.at[phase, 1])
        x_wait(13, phase, pair_in.at[phase, 3])
        for direction, near, keep in ((0, 1, high), (1, 3, low)):
            side_out[direction, 1] = pair_sum(near, keep).astype(BF16)
        acc[0] = block(0, core)
        for direction in (0, 1):
            side_start(phase, direction, 1)
        for near, keep in ((1, low), (3, high)):
            acc[near, keep, :] = pair_sum(near, keep)
        x_wait(10, phase, pair_in.at[phase, 0])
        res[...] = res[...] + factor * (acc[0] + pair_in[phase, 0].astype(F32))

    def side_start(phase, direction, order):
        x_start(
            14 + 2 * order + direction, phase, side_out.at[direction, order], side_in.at[phase, direction, order],
            {"tp": ahead if direction == 0 else behind},
        )

    def side_wait(phase, direction, order):
        x_wait(14 + 2 * order + direction, phase, side_in.at[phase, direction, order])

    def merge(phase):
        for direction, near, keep in ((0, 1, low), (1, 3, high)):
            side_wait(phase, direction, 0)
            side_out[direction, 2] = (acc[near, keep, :] + side_in[phase, direction, 0].astype(F32)).astype(BF16)
        for direction in (0, 1):
            side_start(phase, direction, 2)

    def finish(phase, factor):
        for order in (1, 2):
            for direction in (0, 1):
                side_wait(phase, direction, order)
        lo = side_in[phase, 0, 2].astype(F32) + side_in[phase, 1, 1].astype(F32)
        hi = side_in[phase, 0, 1].astype(F32) + side_in[phase, 1, 2].astype(F32)
        target = out if phase == 2 else raw.at[phase + 1, t]
        for keep, extra in ((low, lo), (high, hi)):
            target[keep, :] = (res[keep, :] + factor * extra).astype(BF16)
        if phase < 2:
            for keep, extra in ((low, lo), (high, hi)):
                res[keep, :] = res[keep, :] + factor * extra
            ag_start(phase + 1)

    def norm0():
        norm(0, gain_first)
        res[...] = raw[0, t].astype(F32)

    stages = {
        "ag_start0": lambda: ag_start(0), "ag_pass0": lambda: ag_pass(0), "ag_mid0": lambda: ag_mid(0),
        "ag_far0": lambda: ag_far(0), "norm0": norm0,
        "hidden1a": lambda: hidden_stage("g1", "u1", 0, 2), "hidden1b": lambda: hidden_stage("g1", "u1", 3, 4),
        "hidden1c": lambda: hidden_stage("g1", "u1", 5, 6), "hidden1d": lambda: hidden_stage("g1", "u1", 7, half),
        "branch0": lambda: branch(0, hidden, "d1", 0, 0.5), "merge0": lambda: merge(0),
        "finish0": lambda: finish(0, 0.5),
        "ag_pass1": lambda: ag_pass(1), "ag_mid1": lambda: ag_mid(1),
        "ag_far1": lambda: ag_far(1),
        "norm1": lambda: norm(1, gain_mixer), "mixer": mixer,
        "branch1": lambda: branch(1, mixed, "mx", 3 * depth, 1.0), "merge1": lambda: merge(1),
        "finish1": lambda: finish(1, 1.0),
        "ag_pass2": lambda: ag_pass(2), "ag_mid2": lambda: ag_mid(2),
        "ag_far2": lambda: ag_far(2),
        "norm2": lambda: norm(2, gain_last), "hidden2a": lambda: hidden_stage("g2", "u2", 0, 6),
        "hidden2c": lambda: hidden_stage("g2", "u2", 7, half),
        "branch2": lambda: branch(2, hidden, "d2", 0, 0.5), "merge2": lambda: merge(2),
        "finish2": lambda: finish(2, 0.5),
    }

    plan = plan_for(half)
    for event in ring_order(half):
        with jax.named_scope("ring_%s_%d" % event):
            ring_event(*event)
        for stage in plan.get(event, ()):
            with jax.named_scope(stage):
                stages[stage]()

    for copy in list(x_flight.values()):
        copy.wait_send()
    for key, queue in in_flight.items():
        if isinstance(queue, list):
            for copy in queue:
                copy.wait_send()


def ring_order(half):
    events = []
    lead = half // 2 - 1
    for hop in range(half + 1):
        events += [(name, hop) for name in ("d1", "g1", "u1")]
        if lead <= hop < half:
            events.append(("mx", hop - lead))
        if hop == half - 1:
            events += [(name, 0) for name in ("g2", "u2", "d2")]
    late = [(name, hop) for hop in range(1, half + 1) for name in ("g2", "u2", "d2")]
    for hop in range(half - lead, half + 1):
        events.append(("mx", hop))
        for _ in range(MIXED[hop - half + lead] if half == 8 else 2):
            events.append(late.pop(0))
    return events + late


def plan_for(half):
    events = ring_order(half)
    plan = {}
    if half != 8:
        every = [stage for _, _, stages in EARLY for stage in stages] + [stage for _, stage in LATE]
        plan[events[-1]] = tuple(every) + LAST
        return plan
    for anchor, offset, stages in EARLY:
        plan.setdefault(events[events.index(anchor) + offset], []).extend(stages)
    base = events.index(("u1", half))
    for offset, stage in LATE:
        plan.setdefault(events[base + offset], []).append(stage)
    plan.setdefault(events[-1], []).extend(LAST)
    return plan


def fused_layer(n_fs, n_tp, n_grp, *args):
    tokens, gate, down, outer = args[0], args[2], args[4], args[6]
    rows, cols = tokens.shape
    paired = n_grp % 2 == 0
    n_x = n_tp // 2
    depth, hid = gate.shape
    chan = outer.shape[1]

    def split(length, share):
        alone = own_part(length, share) if paired else 0
        return alone, length - 2 * alone

    splits = {
        "g1": split(depth, 0.38), "u1": split(depth, 0.3), "d1": split(hid, 0.35), "mx": split(4 * depth, 0.38),
        "g2": split(depth, 0.3), "u2": split(depth, 0.3), "d2": split(hid, 0.38),
    }
    half = n_fs // 2
    wide = pltpu.VMEM((n_fs, depth, hid), BF16)
    tall = pltpu.VMEM((n_fs, hid, depth), BF16)
    gains = {1, 5, 11}
    args = [a.reshape(1, -1) if i in gains else a for i, a in enumerate(args)]
    vmem, anywhere = pl.BlockSpec(memory_space=pltpu.VMEM), pl.BlockSpec(memory_space=pl.ANY)
    in_vmem = gains | {9}
    return pl.pallas_call(
        functools.partial(layer, (n_fs, n_tp, paired, splits)),
        out_shape=jax.ShapeDtypeStruct((rows, cols), BF16),
        in_specs=[vmem if i in in_vmem else anywhere for i in range(len(args))],
        out_specs=vmem,
        scratch_shapes=[
            wide, wide, tall, pltpu.VMEM((n_fs, 4 * depth, chan), BF16), wide, wide, tall,
            pltpu.VMEM((3, n_tp, rows, cols), BF16),
            pltpu.VMEM((n_fs, rows, depth), BF16),
            pltpu.VMEM((hid // 128, rows, 256), F32),
            pltpu.VMEM((rows, hid), BF16),
            pltpu.VMEM((rows, chan), BF16),
            pltpu.VMEM((rows, cols), F32),
            pltpu.VMEM((n_x, rows, cols), F32),
            pltpu.VMEM((n_x, rows, cols), BF16),
            pltpu.VMEM((3, n_x, rows, cols), BF16),
            pltpu.VMEM((2, 3, rows // 2, cols), BF16),
            pltpu.VMEM((3, 2, 3, rows // 2, cols), BF16),
            pltpu.SemaphoreType.DMA((11,)),
            pltpu.SemaphoreType.DMA((2, 4)),
            pltpu.SemaphoreType.DMA((7, 2, half)),
            pltpu.SemaphoreType.DMA((4,)),
            pltpu.SemaphoreType.DMA((7, half // 2)),
            pltpu.SemaphoreType.DMA((20,)),
            pltpu.SemaphoreType.DMA((2, 20)),
        ],
        compiler_params=pltpu.CompilerParams(
            collective_id=0, has_side_effects=True, vmem_limit_bytes=60 * 1024 * 1024
        ),
        name="fused_layer",
    )(*args)


def solution(mesh):
    in_specs = (
        P(("grp", "fs"), "tp"),
        P(),
        P("fs", "tp"),
        P("fs", "tp"),
        P("tp", "fs"),
        P(),
        P("fs", "tp"),
        P("fs", "tp"),
        P("fs", "tp"),
        P(None, "tp"),
        P("tp", "fs"),
        P(),
        P("fs", "tp"),
        P("fs", "tp"),
        P("tp", "fs"),
    )
    out_specs = P(("grp", "fs"), "tp")
    body = functools.partial(fused_layer, mesh.shape["fs"], mesh.shape["tp"], mesh.shape["grp"])
    return jax.shard_map(body, mesh=mesh, in_specs=in_specs, out_specs=out_specs, check_vma=False)
```
